512 devices in a mesh: grp: 2 (over y), tp: 16 (over z), dp: 16 (over x, core).
Axes of the slice: x: 8, y: 2, z: 16, core: 2. Of those that a mesh axis runs over, the one named last changes fastest.
The devices are a block of a 8x16x16 slice.
Arguments:
- tokens: bfloat16 [1024, 4096], P(('grp', 'tp'), 'dp'), parts along dimension 0, may hold values from -6 to 6
- lengths: int32 [256], P(('grp', 'dp')), parts along dimension 0, may hold values from 1 to 4, as said below
- norm_gain: float32 [2, 4096], P(None, 'dp'), may hold values from 0.1 to 1.9
- w_recept: bfloat16 [2, 4096, 2048], P(None, 'dp', 'tp'), may hold values from -0.09375 to 0.09375
- w_keys: bfloat16 [2, 4096, 2048], P(None, 'dp', 'tp'), may hold values from -0.09375 to 0.09375
- w_values: bfloat16 [2, 4096, 2048], P(None, 'dp', 'tp'), may hold values from -0.09375 to 0.09375
- w_decay: bfloat16 [2, 4096, 2048], P(None, 'dp', 'tp'), may hold values from -0.09375 to 0.09375
- w_rate: bfloat16 [2, 4096, 2048], P(None, 'dp', 'tp'), may hold values from -0.09375 to 0.09375
- w_gate: bfloat16 [2, 4096, 2048], P(None, 'dp', 'tp'), may hold values from -0.09375 to 0.09375
- decay_base: float32 [2, 2048], P(None, 'tp'), may hold values from -3 to 1
- group_gain: float32 [2, 2048], P(None, 'tp'), may hold values from 0.1 to 1.9
- w_out: bfloat16 [2, 2048, 4096], P(None, 'tp', 'dp'), may hold values from -0.125 to 0.125
- states: float32 [2, 256, 32, 4096], P(None, ('grp', 'dp'), 'tp'), parts along dimension 1, may hold values from -2 to 2
Outputs:
- tokens_out: bfloat16 [1024, 4096], P(('grp', 'tp'), 'dp'), parts along dimension 0
- states_out: float32 [2, 256, 32, 4096], P(None, ('grp', 'dp'), 'tp'), parts along dimension 1
The draws below stay inside these ranges and needn't reach their ends.
There are 2 independent parts, one for each index of `grp`. The reference program is written for one: setup_inputs(seed, part) draws one part's arguments, and reference() takes and returns one part's arrays. A program takes and returns all parts, laid end to end along the dimension named above; an argument that names none is the same for every part. Nothing has to cross between parts.
Inputs may be any that keep to these rules, and one draw needn't show every extreme that they name: Sequence s has its first lengths[s] of its 4 slots live; in every draw all 8 sequences of some index of dp have 4 live slots.
All inputs are finite; a program needn't handle non-finite values.
Results may differ from the reference program's by a relative error of at most 0.029.
Values may be sent and summed in bfloat16 or wider, within the bound.
A program may use at most 64 MiB of HBM per device.

```python
import jax
import jax.numpy as jnp
from jax import lax

D = 4096
HEADS = 32
HEAD = 64
NEW = 4
SEQ_DEV = 8
WIDTH = 2048
SEQS = 128
TOKENS = 512


def draw_lengths(key, part):
    key_ticket = jax.random.fold_in(key, 11)
    key_block = jax.random.fold_in(key, 12)
    ticket = jax.random.randint(key_ticket, (SEQS,), 0, 100)
    length_base = 1 + (ticket >= 55).astype(jnp.int32) + (ticket >= 85).astype(jnp.int32) + (ticket >= 93).astype(jnp.int32)
    length_base = jnp.minimum(length_base, NEW)
    chosen = jax.random.randint(key_block, (), 0, SEQS // SEQ_DEV)
    owner_block = jnp.arange(SEQS, dtype=jnp.int32) // SEQ_DEV
    return jnp.where(owner_block == chosen, NEW, length_base).astype(jnp.int32)


def block_levels(key, extent, cuts, low, high):
    def one(dim, blocks):
        heights = jax.random.uniform(jax.random.fold_in(jax.random.fold_in(key, 6), dim), (blocks,), jnp.float32, low / len(cuts), high / len(cuts))
        return jnp.repeat(jnp.exp(heights), extent[dim] // blocks).reshape((-1,) + (1,) * (len(extent) - dim - 1))

    gain = one(*cuts[0])
    for cut in cuts[1:]:
        gain = gain * one(*cut)
    return gain


def scatter_about(key, shape, spread, bound, split=(), kind=jnp.bfloat16):
    drawn = spread * jax.random.normal(key, shape, jnp.float32)
    if split:
        drawn = drawn * block_levels(key, shape, split, -0.22, 0.18)
    return jnp.clip(drawn, -bound, bound).astype(kind)


def setup_inputs(seed: int = 0, part: int = 0) -> dict:
    seeds = jax.random.split(jax.random.key(seed), 14)
    part_splits = jax.random.split(jax.random.fold_in(seeds[13], part), 14)
    tokens = scatter_about(part_splits[0], (TOKENS, D), 1.0, 6.0, ((0, 16), (1, 16)))
    lengths = draw_lengths(jax.random.fold_in(jax.random.fold_in(seeds[13], part), 71), part)
    norm_gain = jnp.clip(1.0 + 0.18 * jax.random.normal(seeds[2], (2, D), jnp.float32), 0.1, 1.9)
    w_recept = scatter_about(seeds[3], (2, D, WIDTH), D ** -0.5, 0.09375, ((1, 16), (2, 16)))
    w_keys = scatter_about(seeds[4], (2, D, WIDTH), D ** -0.5, 0.09375, ((1, 16), (2, 16)))
    w_values = scatter_about(seeds[5], (2, D, WIDTH), D ** -0.5, 0.09375, ((1, 16), (2, 16)))
    w_decay = scatter_about(seeds[6], (2, D, WIDTH), D ** -0.5, 0.09375, ((1, 16), (2, 16)))
    w_rate = scatter_about(seeds[7], (2, D, WIDTH), D ** -0.5, 0.09375, ((1, 16), (2, 16)))
    w_gate = scatter_about(seeds[8], (2, D, WIDTH), D ** -0.5, 0.09375, ((1, 16), (2, 16)))
    decay_base = jnp.clip(-3.0 + 4.0 * jax.random.uniform(seeds[9], (2, WIDTH), jnp.float32) ** block_levels(seeds[9], (2, WIDTH), ((1, 16),), -0.2, 0.2), -3.0, 1.0)
    group_gain = jnp.clip(1.0 + 0.18 * jax.random.normal(seeds[10], (2, WIDTH), jnp.float32), 0.1, 1.9)
    w_out = scatter_about(seeds[11], (2, WIDTH, D), WIDTH ** -0.5, 0.125, ((1, 16), (2, 16)))
    states = scatter_about(part_splits[12], (2, SEQS, HEADS, HEAD * HEAD), 0.3, 2.0, ((1, 16), (2, 16)), jnp.float32)
    return dict(tokens=tokens, lengths=lengths, norm_gain=norm_gain, w_recept=w_recept, w_keys=w_keys, w_values=w_values, w_decay=w_decay, w_rate=w_rate, w_gate=w_gate, decay_base=decay_base, group_gain=group_gain, w_out=w_out, states=states)


norm_epsilon = 1e-06
unit_epsilon = 0.00064
group_epsilon = 0.00064

def advance(state_in, pieces, lengths, base_log, gain_vec):
    seq_count = state_in.shape[0]
    head_count = state_in.shape[1]
    head_shape = (seq_count, NEW, head_count, HEAD)
    recept, keys, values, decay_pre, rate_pre, gate_pre = [piece.astype(jnp.float32).reshape(head_shape) for piece in pieces]
    decays = jnp.exp(-jnp.exp(-jax.nn.softplus(-(base_log.reshape(head_count, HEAD) + decay_pre)) - 0.5))
    rates = jax.nn.sigmoid(rate_pre)
    unit_keys = keys * lax.rsqrt(lax.optimization_barrier(jnp.sum(keys * keys, -1, keepdims=True)) + unit_epsilon)
    memory = state_in.reshape(seq_count, head_count, HEAD, HEAD)
    live_mask = jnp.arange(NEW)[None, :] < lengths[:, None]
    readings = []
    for position in range(NEW):
        unit_now = unit_keys[:, position]
        removed = jnp.einsum('shvk,shk->shv', memory, unit_now)
        updated = memory * decays[:, position][:, :, None, :] - removed[..., None] * (unit_now * rates[:, position])[:, :, None, :] + values[:, position][..., None] * keys[:, position][:, :, None, :]
        live_now = live_mask[:, position][:, None, None, None]
        memory = jnp.where(live_now, updated, memory)
        readings.append(jnp.einsum('shvk,shk->shv', memory, recept[:, position]))
    outputs_h = jnp.stack(readings, 1)
    head_mean = lax.optimization_barrier(jnp.mean(outputs_h, -1, keepdims=True))
    head_var = lax.optimization_barrier(jnp.mean(jnp.square(outputs_h - head_mean), -1, keepdims=True))
    normed = (outputs_h - head_mean) * lax.rsqrt(head_var + group_epsilon) * gain_vec.reshape(head_count, HEAD)
    mixed_out = normed * jax.nn.sigmoid(gate_pre) * live_mask[:, :, None, None].astype(jnp.float32)
    return (memory.reshape(state_in.shape), mixed_out.reshape(seq_count * NEW, head_count * HEAD).astype(jnp.bfloat16))

def reference(tokens, lengths, norm_gain, w_recept, w_keys, w_values, w_decay, w_rate, w_gate, decay_base, group_gain, w_out, states):
    current = tokens
    new_states = []
    for layer_id in range(2):
        wide_rows = current.astype(jnp.float32)
        inv_rms = lax.rsqrt(lax.optimization_barrier(jnp.sum(wide_rows * wide_rows, -1, keepdims=True)) / D + norm_epsilon)
        scaled = (wide_rows * norm_gain[layer_id]).astype(jnp.bfloat16)
        pieces = [(inv_rms * jnp.dot(scaled, matrix[layer_id], preferred_element_type=jnp.float32)).astype(jnp.bfloat16) for matrix in (w_recept, w_keys, w_values, w_decay, w_rate, w_gate)]
        memory, mixed_out = advance(states[layer_id], pieces, lengths, decay_base[layer_id], group_gain[layer_id])
        new_states.append(memory)
        current = (wide_rows + jnp.dot(mixed_out, w_out[layer_id], preferred_element_type=jnp.float32)).astype(jnp.bfloat16)
    return (current, jnp.stack(new_states))
```

```python
import functools

import jax
import jax.numpy as jnp
from jax import lax
from jax.experimental import pallas as pl
from jax.experimental.pallas import tpu as pltpu
from jax.sharding import PartitionSpec as P

HEAD = 64
NEW = 4
LANES = 128
norm_epsilon = 1e-06
unit_epsilon = 0.00064
group_epsilon = 0.00064
MESH = pl.DeviceIdType.MESH
F32 = jnp.float32
BF16 = jnp.bfloat16


def iota(shape, dim):
    return lax.broadcasted_iota(jnp.int32, shape, dim)


def dot(a, b):
    return jnp.dot(a, b, preferred_element_type=F32)


def dot_split(a, b):
    high = a.astype(BF16)
    low = (a - high.astype(F32)).astype(BF16)
    return dot(high, b) + dot(low, b)


def pair_rows(value):
    high = value.astype(BF16).astype(F32)
    return jnp.concatenate([high, value - high], axis=-2)


def by_distance(n, act):
    act(n // 2)

    def body(step, carry):
        dist = n // 2 - 1 - step
        act(dist)
        act(n - dist)
        return carry

    lax.fori_loop(0, n // 2 - 1, body, 0)


def kernel(
    n_tp, n_dp,
    tokens_ref, lengths_ref, gain_ref, base_ref, group_ref,
    w0, w1, w2, w3, w4, w5, wout_hbm, states_hbm,
    tokens_out, states_out,
    w_v, wo_v, st_v, x_buf, pair_out, pair_in, own_part, rs_out, rs_in, mix_buf, part_out, part_in,
    local_sem, st_sem, z_send, z_recv, d_send, d_recv, rs_send, rs_recv, pair_send, pair_recv,
):
    t = lax.axis_index("tp")
    d = lax.axis_index("dp")
    n_x = n_dp // 2
    x = d // 2
    c = d % 2
    rows = tokens_ref.shape[0]
    feats = tokens_ref.shape[1]
    seqs = rows // NEW
    width = LANES
    model = feats * n_dp

    loads = []
    for i, w in enumerate((w0, w1, w2, w3, w4, w5)):
        loads.append(
            pltpu.make_async_copy(w, w_v.at[:, :, pl.ds(i * width, width)], local_sem.at[i])
        )
    loads.append(pltpu.make_async_copy(wout_hbm, wo_v, local_sem.at[6]))
    loads.append(pltpu.make_async_copy(states_hbm, st_v, local_sem.at[7]))
    for load in loads:
        load.start()

    barrier = pltpu.get_barrier_semaphore()

    def greet_z(off):
        pl.semaphore_signal(barrier, inc=1, device_id={"tp": lax.rem(t + off, n_tp)}, device_id_type=MESH)

    def greet_d(off):
        pl.semaphore_signal(barrier, inc=1, device_id={"dp": lax.rem(d + off, n_dp)}, device_id_type=MESH)

    by_distance(n_tp, greet_z)
    by_distance(n_dp, greet_d)
    pl.semaphore_wait(barrier, n_tp + n_dp - 2)

    def z_copy(src, dst_of, phase, peer, slot):
        return pltpu.make_async_remote_copy(
            src_ref=src, dst_ref=dst_of(slot),
            send_sem=z_send.at[phase, peer], recv_sem=z_recv.at[phase, slot],
            device_id={"tp": peer}, device_id_type=MESH,
        )

    def d_copy(layer, peer, slot):
        return pltpu.make_async_remote_copy(
            src_ref=mix_buf.at[layer, d], dst_ref=mix_buf.at[layer, slot],
            send_sem=d_send.at[layer, peer], recv_sem=d_recv.at[layer, slot],
            device_id={"dp": peer}, device_id_type=MESH,
        )

    def rs_copy(layer, peer, slot):
        return pltpu.make_async_remote_copy(
            src_ref=rs_out.at[layer, peer], dst_ref=rs_in.at[layer, slot],
            send_sem=rs_send.at[layer, peer], recv_sem=rs_recv.at[layer, slot],
            device_id={"dp": peer * 2 + c}, device_id_type=MESH,
        )

    def pair_copy(layer):
        return pltpu.make_async_remote_copy(
            src_ref=pair_out.at[layer], dst_ref=pair_in.at[layer],
            send_sem=pair_send.at[layer], recv_sem=pair_recv.at[layer],
            device_id={"dp": x * 2 + (1 - c)}, device_id_type=MESH,
        )

    def x_slot(layer):
        return lambda slot: x_buf.at[layer, slot // 2, slot % 2]

    def part_slot(layer):
        return lambda slot: part_in.at[layer, slot]

    lane8 = iota((8, LANES), 1)
    m8 = (lane8 // HEAD) == (iota((8, LANES), 0) % 2)
    sq = (LANES, LANES)
    same_half = ((iota(sq, 0) // HEAD) == (iota(sq, 1) // HEAD)).astype(F32).astype(BF16)
    spread = ((iota(sq, 0) % 2) == (iota(sq, 1) // HEAD)).astype(F32).astype(BF16)
    collect = ((iota(sq, 0) // HEAD) == (iota(sq, 1) % 2)).astype(F32).astype(BF16)
    tall = (HEAD, LANES)
    row_of = iota(tall, 0)
    lane_of = iota(tall, 1)
    entry = (((lane_of // HEAD) == (row_of % 2)) & (((lane_of % HEAD) // 2) == (row_of // 2))).astype(F32)
    entry = entry.reshape(1, 8, 8, LANES)
    tok_row = iota((rows, LANES), 0)
    length_rows = jnp.zeros((rows, LANES), jnp.int32)
    for s in range(seqs):
        length_rows = jnp.where((tok_row // NEW) == s, lengths_ref[s], length_rows)
    live = (tok_row % NEW) < length_rows

    def send_tokens(off):
        z_copy(tokens_ref, x_slot(0), 0, lax.rem(t + off, n_tp), t).start()

    by_distance(n_tp, send_tokens)
    x_buf[0, t // 2, t % 2] = tokens_ref[...]
    own_rows = tokens_ref[...].astype(F32)

    def project(layer, half):
        block = x_buf[layer, :, half]
        wide = block.reshape(n_x * rows, feats).astype(F32)
        total = jnp.sum(wide * wide, axis=-1, keepdims=True)
        total = jnp.broadcast_to(total, (n_x * rows, LANES)).reshape(n_x, rows // 8, 8, LANES)
        group = lane8 // 32
        packed = jnp.where(
            group == 0, total[:, 0],
            jnp.where(group == 1, total[:, 1], jnp.where(group == 2, total[:, 2], total[:, 3])),
        )
        scaled = (wide * gain_ref[pl.ds(layer, 1), :]).astype(BF16)
        return scaled, packed

    for layer in range(2):
        def wait_tokens(off):
            src = lax.rem(t + off, n_tp)
            z_copy(tokens_ref, x_slot(layer), 2 * layer, t, src).wait_recv()

        by_distance(n_tp, wait_tokens)
        if layer == 0:
            for load in loads:
                load.wait()

        scaled, packed = project(layer, 1 - c)
        for j in range(3):
            out = dot(scaled, w_v[layer, :, 2 * width * j : 2 * width * (j + 1)])
            for k in range(2):
                i = 2 * j + k
                piece = out[:, k * width : (k + 1) * width].astype(BF16)
                pair_out[layer, :, i * rows : (i + 1) * rows, :] = piece.reshape(n_x, rows, width)
        pair_out[layer, :, 6 * rows : 6 * rows + 16, :] = pair_rows(packed).astype(BF16)
        pair_copy(layer).start()

        scaled, packed = project(layer, c)
        for j in range(3):
            out = dot(scaled, w_v[layer, :, 2 * width * j : 2 * width * (j + 1)])
            for k in range(2):
                i = 2 * j + k
                own_part[:, i * rows : (i + 1) * rows, :] = out[:, k * width : (k + 1) * width].reshape(n_x, rows, width)
        own_part[:, 6 * rows : 6 * rows + 8, :] = packed
        pair_copy(layer).wait_recv()

        def both(place):
            arrived = pair_in[layer, place].astype(F32)
            main = own_part[place, : 6 * rows] + arrived[: 6 * rows]
            squares = own_part[place, 6 * rows : 6 * rows + 8] + (
                arrived[6 * rows : 6 * rows + 8] + arrived[6 * rows + 8 :]
            )
            return main, squares

        def send_sums(off):
            place = lax.rem(x + off, n_x)
            main, squares = both(place)
            rs_out[layer, place, : 6 * rows] = main.astype(BF16)
            rs_out[layer, place, 6 * rows :] = pair_rows(squares).astype(BF16)
            rs_copy(layer, place, x).start()

        by_distance(n_x, send_sums)
        main, squares = both(x)
        own_part[x, : 6 * rows] = main
        own_part[x, 6 * rows : 6 * rows + 8] = squares

        def add_sums(off):
            src = lax.rem(x + off, n_x)
            rs_copy(layer, x, src).wait_recv()
            arrived = rs_in[layer, src].astype(F32)
            own_part[x, : 6 * rows] += arrived[: 6 * rows]
            own_part[x, 6 * rows : 6 * rows + 8] += arrived[6 * rows : 6 * rows + 8] + arrived[6 * rows + 8 :]

        by_distance(n_x, add_sums)

        squares = own_part[x, 6 * rows : 6 * rows + 8]
        inv = lax.rsqrt(squares / model + norm_epsilon)
        inv_rows = jnp.concatenate(
            [jnp.broadcast_to(inv[:, 32 * g : 32 * g + 1], (8, LANES)) for g in range(rows // 8)], 0
        )
        recept, keys, values, decay_pre, rate_pre, gate_pre = [
            (inv_rows * own_part[x, i * rows : (i + 1) * rows]).astype(BF16).astype(F32) for i in range(6)
        ]
        raw = base_ref[pl.ds(layer, 1), :] + decay_pre
        decays = jnp.exp(-jnp.exp(jnp.float32(-0.5)) / (1.0 + jnp.exp(-raw)))
        rates = 1.0 / (1.0 + jnp.exp(-rate_pre))
        unit = keys * lax.rsqrt(dot_split(keys * keys, same_half) + unit_epsilon)
        zero = jnp.zeros_like(keys)
        decays = jnp.where(live, decays, 1.0)
        drop = jnp.where(live, unit * rates, zero)
        put = jnp.where(live, keys, zero)

        def tile_maker(q):
            turned = pltpu.roll(q, HEAD, 1)

            def tiles(n):
                made = []
                for s in range(seqs):
                    at = NEW * s + n
                    made.append(
                        jnp.where(
                            m8,
                            jnp.broadcast_to(q[at : at + 1], (8, LANES)),
                            jnp.broadcast_to(turned[at : at + 1], (8, LANES)),
                        )
                    )
                return jnp.stack(made)[:, None]

            return tiles

        decay_tiles, unit_tiles, drop_tiles, put_tiles, recept_tiles = [
            tile_maker(q) for q in (decays, unit, drop, put, recept)
        ]
        full = (seqs, 8, 8, LANES)
        flat = (seqs * HEAD, LANES)
        memory = st_v[layer].reshape(full)
        reads = jnp.zeros((rows, LANES), F32)
        for n in range(NEW):
            value_rows = jnp.stack(
                [jnp.broadcast_to(values[NEW * s + n : NEW * s + n + 1], (8, LANES)) for s in range(seqs)]
            )[:, None]
            value_full = dot((value_rows * entry).reshape(flat).astype(BF16), spread).reshape(full)
            removed = dot_split((memory * unit_tiles(n)).reshape(flat), same_half).reshape(full)
            memory = memory * decay_tiles(n) - removed * drop_tiles(n) + value_full * put_tiles(n)
            seen = dot_split((memory * recept_tiles(n)).reshape(flat), collect).reshape(full)
            seen = jnp.sum(seen * entry, axis=1).reshape(seqs * 8, LANES)
            pick_shape = (rows, seqs * 8)
            pick = (iota(pick_shape, 0) == (iota(pick_shape, 1) // 8) * NEW + n).astype(F32).astype(BF16)
            seen_high = seen.astype(BF16)
            seen_low = (seen - seen_high.astype(F32)).astype(BF16)
            reads = reads + dot(pick, seen_high) + dot(pick, seen_low)
        st_v[layer] = memory.reshape(flat)
        pltpu.make_async_copy(st_v.at[layer], states_out.at[layer], st_sem.at[layer]).start()

        mean = dot_split(reads, same_half) / HEAD
        dev = reads - mean
        var = dot_split(dev * dev, same_half) / HEAD
        normed = dev * lax.rsqrt(var + group_epsilon) * group_ref[pl.ds(layer, 1), :]
        mixed = jnp.where(live, normed / (1.0 + jnp.exp(-gate_pre)), zero)
        mix_buf[layer, d] = mixed.astype(BF16)

        def send_mixed(off):
            d_copy(layer, lax.rem(d + off, n_dp), d).start()

        def wait_mixed(off):
            d_copy(layer, d, lax.rem(d + off, n_dp)).wait_recv()

        by_distance(n_dp, send_mixed)
        by_distance(n_dp, wait_mixed)
        partial = dot(mix_buf[layer].reshape(n_dp * rows, width), wo_v[layer])
        part_out[layer] = partial.astype(BF16).reshape(n_tp, rows, feats)

        def send_part(off):
            peer = lax.rem(t + off, n_tp)
            z_copy(part_out.at[layer, peer], part_slot(layer), 2 * layer + 1, peer, t).start()

        by_distance(n_tp, send_part)
        part_in[layer, t] = part_out[layer, t]

        def wait_part(off):
            src = lax.rem(t + off, n_tp)
            z_copy(part_out.at[layer, t], part_slot(layer), 2 * layer + 1, t, src).wait_recv()

        by_distance(n_tp, wait_part)
        own_rows = own_rows + jnp.sum(part_in[layer].astype(F32), axis=0)
        own_rows = own_rows.astype(BF16)
        if layer == 0:
            x_buf[1, t // 2, t % 2] = own_rows

            def send_rows(off):
                z_copy(x_buf.at[1, t // 2, t % 2], x_slot(1), 2, lax.rem(t + off, n_tp), t).start()

            by_distance(n_tp, send_rows)
            own_rows = own_rows.astype(F32)
        else:
            tokens_out[...] = own_rows

    for layer in range(2):
        def drain_z(off):
            peer = lax.rem(t + off, n_tp)
            z_copy(tokens_ref, x_slot(layer), 2 * layer, peer, t).wait_send()
            z_copy(part_out.at[layer, peer], part_slot(layer), 2 * layer + 1, peer, t).wait_send()

        def drain_d(off):
            d_copy(layer, lax.rem(d + off, n_dp), d).wait_send()

        def drain_rs(off):
            rs_copy(layer, lax.rem(x + off, n_x), x).wait_send()

        by_distance(n_tp, drain_z)
        by_distance(n_dp, drain_d)
        by_distance(n_x, drain_rs)
        pair_copy(layer).wait_send()
        pltpu.make_async_copy(st_v.at[layer], states_out.at[layer], st_sem.at[layer]).wait()


def per_device(n_tp, n_dp, tokens, lengths, norm_gain, w_recept, w_keys, w_values, w_decay, w_rate, w_gate,
               decay_base, group_gain, w_out, states):
    rows, feats = tokens.shape
    layers, seqs, heads, flat = states.shape
    folded = flat // LANES
    width = w_recept.shape[2]
    n_x = n_dp // 2
    state_rows = seqs * folded * heads
    packed = states.reshape(layers, seqs, heads, folded, LANES).transpose(0, 1, 3, 2, 4)
    packed = packed.reshape(layers, state_rows, LANES)
    vmem = pl.BlockSpec(memory_space=pltpu.VMEM)
    hbm = pl.BlockSpec(memory_space=pltpu.HBM)
    msg = 6 * rows + 16
    out, new_states = pl.pallas_call(
        functools.partial(kernel, n_tp, n_dp),
        out_shape=(
            jax.ShapeDtypeStruct((rows, feats), BF16),
            jax.ShapeDtypeStruct((layers, state_rows, LANES), F32),
        ),
        in_specs=[vmem, pl.BlockSpec(memory_space=pltpu.SMEM), vmem, vmem, vmem] + [hbm] * 8,
        out_specs=(vmem, hbm),
        scratch_shapes=[
            pltpu.VMEM((layers, feats, 6 * width), BF16),
            pltpu.VMEM((layers, width, feats), BF16),
            pltpu.VMEM((layers, state_rows, LANES), F32),
            pltpu.VMEM((layers, n_tp // 2, 2, rows, feats), BF16),
            pltpu.VMEM((layers, n_x, msg, width), BF16),
            pltpu.VMEM((layers, n_x, msg, width), BF16),
            pltpu.VMEM((n_x, msg, width), F32),
            pltpu.VMEM((layers, n_x, msg, width), BF16),
            pltpu.VMEM((layers, n_x, msg, width), BF16),
            pltpu.VMEM((layers, n_dp, rows, width), BF16),
            pltpu.VMEM((layers, n_tp, rows, feats), BF16),
            pltpu.VMEM((layers, n_tp, rows, feats), BF16),
            pltpu.SemaphoreType.DMA((8,)),
            pltpu.SemaphoreType.DMA((2,)),
            pltpu.SemaphoreType.DMA((4, n_tp)),
            pltpu.SemaphoreType.DMA((4, n_tp)),
            pltpu.SemaphoreType.DMA((2, n_dp)),
            pltpu.SemaphoreType.DMA((2, n_dp)),
            pltpu.SemaphoreType.DMA((2, n_x)),
            pltpu.SemaphoreType.DMA((2, n_x)),
            pltpu.SemaphoreType.DMA((2,)),
            pltpu.SemaphoreType.DMA((2,)),
        ],
        compiler_params=pltpu.CompilerParams(
            collective_id=0, has_side_effects=True, vmem_limit_bytes=48 * 1024 * 1024
        ),
    )(tokens, lengths, norm_gain, decay_base, group_gain,
      w_recept, w_keys, w_values, w_decay, w_rate, w_gate, w_out, packed)
    new_states = new_states.reshape(layers, seqs, folded, heads, LANES).transpose(0, 1, 3, 2, 4)
    return out, new_states.reshape(layers, seqs, heads, flat)


def solution(mesh):
    placed = (
        P(("grp", "tp"), "dp"),
        P(("grp", "dp")),
        P(None, "dp"),
        P(None, "dp", "tp"),
        P(None, "dp", "tp"),
        P(None, "dp", "tp"),
        P(None, "dp", "tp"),
        P(None, "dp", "tp"),
        P(None, "dp", "tp"),
        P(None, "tp"),
        P(None, "tp"),
        P(None, "tp", "dp"),
        P(None, ("grp", "dp"), "tp", None),
    )
    return jax.shard_map(
        functools.partial(per_device, mesh.shape["tp"], mesh.shape["dp"]),
        mesh=mesh,
        in_specs=placed,
        out_specs=(P(("grp", "tp"), "dp"), P(None, ("grp", "dp"), "tp", None)),
        check_vma=False,
    )
```

```python
import functools

import jax
import jax.numpy as jnp
from jax import lax
from jax.experimental import pallas as pl
from jax.experimental.pallas import tpu as pltpu
from jax.sharding import PartitionSpec as P

HEAD = 64
NEW = 4
LANES = 128
norm_epsilon = 1e-06
unit_epsilon = 0.00064
group_epsilon = 0.00064
MESH = pl.DeviceIdType.MESH
F32 = jnp.float32
BF16 = jnp.bfloat16


def iota(shape, dim):
    return lax.broadcasted_iota(jnp.int32, shape, dim)


def dot(a, b):
    return jnp.dot(a, b, preferred_element_type=F32)


def dot_split(a, b):
    high = a.astype(BF16)
    low = (a - high.astype(F32)).astype(BF16)
    return dot(high, b) + dot(low, b)


def pair_rows(value):
    high = value.astype(BF16).astype(F32)
    return jnp.concatenate([high, value - high], axis=-2)


def by_distance(n, act):
    act(n // 2)

    def body(step, carry):
        dist = n // 2 - 1 - step
        act(dist)
        act(n - dist)
        return carry

    lax.fori_loop(0, n // 2 - 1, body, 0)


def kernel(
    n_tp, n_dp,
    tokens_hbm, lengths_hbm, gain_hbm, base_hbm, group_hbm,
    w0, w1, w2, w3, w4, w5, wout_hbm, states_hbm,
    tokens_out, states_out,
    tokens_ref, lengths_ref, gain_ref, base_ref, group_ref,
    w_v, wo_v, st_v, x_buf, pair_out, pair_in, own_part, rs_out, rs_in, mix_buf,
    part_out, part_in, class_sum, far_out, far_in,
    local_sem, st_sem, g_send, g_recv, p_send, p_recv, d_send, d_recv, rs_send, rs_recv, pair_send, pair_recv,
):
    t = lax.axis_index("tp")
    d = lax.axis_index("dp")
    n_x = n_dp // 2
    x = d // 2
    c = d % 2
    rows, feats = tokens_ref.shape
    seqs = rows // NEW
    width = LANES
    model = feats * n_dp
    hops = n_tp // 4
    near_first = sorted(range(hops), key=lambda j: min(j, hops - j))
    far_first = near_first[::-1]

    first = pltpu.make_async_copy(tokens_hbm, tokens_ref, local_sem.at[8])
    first.start()
    loads = [
        pltpu.make_async_copy(gain_hbm, gain_ref, local_sem.at[9]),
        pltpu.make_async_copy(base_hbm, base_ref, local_sem.at[10]),
        pltpu.make_async_copy(group_hbm, group_ref, local_sem.at[11]),
        pltpu.make_async_copy(lengths_hbm, lengths_ref, local_sem.at[12]),
    ]
    for i, w in enumerate((w0, w1, w2, w3, w4, w5)):
        loads.append(
            pltpu.make_async_copy(w, w_v.at[:, :, pl.ds(i * width, width)], local_sem.at[i])
        )
    loads.append(pltpu.make_async_copy(wout_hbm, wo_v, local_sem.at[6]))
    loads.append(pltpu.make_async_copy(states_hbm, st_v, local_sem.at[7]))
    for load in loads:
        load.start()

    def around(off):
        return lax.rem(t + off + 2 * n_tp, n_tp)

    skip = 2 - 4 * (t % 2)
    targets = (1, -1, skip)
    sources = (-1, 1, -skip)

    barrier = pltpu.get_barrier_semaphore()

    def greet_z(off):
        pl.semaphore_signal(barrier, inc=1, device_id={"tp": around(off)}, device_id_type=MESH)

    def greet_d(off):
        pl.semaphore_signal(barrier, inc=1, device_id={"dp": lax.rem(d + off, n_dp)}, device_id_type=MESH)

    for j in far_first:
        if j:
            greet_z(4 * j)
    for off in targets + sources[2:]:
        greet_z(off)
    by_distance(n_dp, greet_d)
    first.wait()
    pl.semaphore_wait(barrier, (hops - 1) + 4 + n_dp - 1)

    def g_copy(layer, src, block, peer, k):
        return pltpu.make_async_remote_copy(
            src_ref=src, dst_ref=x_buf.at[layer, block],
            send_sem=g_send.at[layer, k], recv_sem=g_recv.at[layer, block],
            device_id={"tp": peer}, device_id_type=MESH,
        )

    def near_copy(layer, j, i, block, peer):
        return pltpu.make_async_remote_copy(
            src_ref=part_out.at[layer, block], dst_ref=part_in.at[layer, 3 * j + i],
            send_sem=p_send.at[layer, 3 * j + i], recv_sem=p_recv.at[layer, 3 * j + i],
            device_id={"tp": peer}, device_id_type=MESH,
        )

    def far_copy(layer, j, peer):
        return pltpu.make_async_remote_copy(
            src_ref=far_out.at[layer, j], dst_ref=far_in.at[layer, j],
            send_sem=p_send.at[layer, 3 * hops + j - 1], recv_sem=p_recv.at[layer, 3 * hops + j - 1],
            device_id={"tp": peer}, device_id_type=MESH,
        )

    def d_copy(layer, peer, slot):
        return pltpu.make_async_remote_copy(
            src_ref=mix_buf.at[layer, d], dst_ref=mix_buf.at[layer, slot],
            send_sem=d_send.at[layer, peer], recv_sem=d_recv.at[layer, slot],
            device_id={"dp": peer}, device_id_type=MESH,
        )

    def rs_copy(layer, peer, slot):
        return pltpu.make_async_remote_copy(
            src_ref=rs_out.at[layer, peer], dst_ref=rs_in.at[layer, slot],
            send_sem=rs_send.at[layer, peer], recv_sem=rs_recv.at[layer, slot],
            device_id={"dp": peer * 2 + c}, device_id_type=MESH,
        )

    def pair_copy(layer, place):
        return pltpu.make_async_remote_copy(
            src_ref=pair_out.at[layer, place], dst_ref=pair_in.at[layer, place],
            send_sem=pair_send.at[layer, place], recv_sem=pair_recv.at[layer, place],
            device_id={"dp": x * 2 + (1 - c)}, device_id_type=MESH,
        )

    def gather_start(layer, src):
        for j in far_first:
            if j:
                g_copy(layer, src, t, around(4 * j), 3 * hops + j - 1).start()
        for i, off in enumerate(targets):
            g_copy(layer, src, t, around(off), i).start()

    def gather_forward(layer, j):
        block = around(4 * j)
        g_copy(layer, x_buf.at[layer, block], block, t, 0).wait_recv()
        for i, off in enumerate(targets):
            g_copy(layer, x_buf.at[layer, block], block, around(off), 3 * j + i).start()

    def gather_near(layer, j):
        for off in sources:
            block = around(off + 4 * j)
            g_copy(layer, x_buf.at[layer, block], block, t, 0).wait_recv()

    gather_start(0, tokens_ref)
    x_buf[0, t] = tokens_ref[...]
    own_rows = tokens_ref[...].astype(F32)
    for load in loads:
        load.wait()

    lane8 = iota((8, LANES), 1)
    m8 = (lane8 // HEAD) == (iota((8, LANES), 0) % 2)
    sq = (LANES, LANES)
    same_half = ((iota(sq, 0) // HEAD) == (iota(sq, 1) // HEAD)).astype(F32).astype(BF16)
    spread = ((iota(sq, 0) % 2) == (iota(sq, 1) // HEAD)).astype(F32).astype(BF16)
    collect = ((iota(sq, 0) // HEAD) == (iota(sq, 1) % 2)).astype(F32).astype(BF16)
    tall = (HEAD, LANES)
    row_of = iota(tall, 0)
    lane_of = iota(tall, 1)
    entry = (((lane_of // HEAD) == (row_of % 2)) & (((lane_of % HEAD) // 2) == (row_of // 2))).astype(F32)
    entry = entry.reshape(1, 8, 8, LANES)
    tok_row = iota((rows, LANES), 0)
    length_rows = jnp.zeros((rows, LANES), jnp.int32)
    for s in range(seqs):
        length_rows = jnp.where((tok_row // NEW) == s, lengths_ref[s], length_rows)
    live = (tok_row % NEW) < length_rows

    odd = (t + c) % 2
    even = 1 - odd
    mine = (-odd, odd - even * skip)
    theirs = (-even, even - odd * skip)

    def wave(layer, j):
        blocks = [around(off + 4 * j) for off in theirs + mine]
        wide = jnp.concatenate([x_buf[layer, block] for block in blocks], 0).astype(F32)
        total = jnp.sum(wide * wide, axis=-1, keepdims=True)
        total = jnp.broadcast_to(total, (4 * rows, LANES)).reshape(4, rows // 8, 8, LANES)
        group = lane8 // 32
        packed = jnp.where(
            group == 0, total[:, 0],
            jnp.where(group == 1, total[:, 1], jnp.where(group == 2, total[:, 2], total[:, 3])),
        )
        scaled = (wide * gain_ref[pl.ds(layer, 1), :]).astype(BF16)
        for p in range(3):
            out = dot(scaled, w_v[layer, :, 2 * width * p : 2 * width * (p + 1)])
            for k in range(2):
                i = 2 * p + k
                piece = out[:, k * width : (k + 1) * width].reshape(4, rows, width)
                for q in range(2):
                    pair_out[layer, blocks[q] // 2, i * rows : (i + 1) * rows] = piece[q].astype(BF16)
                    own_part[blocks[2 + q] // 2, i * rows : (i + 1) * rows] = piece[2 + q]
        for q in range(2):
            pair_out[layer, blocks[q] // 2, 6 * rows :] = pair_rows(packed[q]).astype(BF16)
            own_part[blocks[2 + q] // 2, 6 * rows : 6 * rows + 8] = packed[2 + q]
        for q in range(2):
            pair_copy(layer, blocks[q] // 2).start()

    def both(layer, place):
        arrived = pair_in[layer, place].astype(F32)
        main = own_part[place, : 6 * rows] + arrived[: 6 * rows]
        squares = own_part[place, 6 * rows : 6 * rows + 8] + (
            arrived[6 * rows : 6 * rows + 8] + arrived[6 * rows + 8 :]
        )
        return main, squares

    def finish(layer, j):
        for off in mine:
            place = around(off + 4 * j) // 2
            pair_copy(layer, place).wait_recv()
            main, squares = both(layer, place)

            @pl.when(place != x)
            def _():
                rs_out[layer, place, : 6 * rows] = main.astype(BF16)
                rs_out[layer, place, 6 * rows :] = pair_rows(squares).astype(BF16)
                rs_copy(layer, place, x).start()

            @pl.when(place == x)
            def _():
                own_part[x, : 6 * rows] = main
                own_part[x, 6 * rows : 6 * rows + 8] = squares

    for layer in range(2):
        gather_near(layer, 0)
        wave(layer, 0)
        for j in near_first[1:-1]:
            gather_forward(layer, j)
        finish(layer, 0)
        for j in near_first[1:][-1:]:
            gather_forward(layer, j)
        for j in near_first[1:-1]:
            gather_near(layer, j)
            wave(layer, j)
        for j in near_first[1:-1]:
            finish(layer, j)
        for j in near_first[1:][-1:]:
            gather_near(layer, j)
            wave(layer, j)
            finish(layer, j)

        def add_sums(off):
            src = lax.rem(x + off, n_x)
            rs_copy(layer, x, src).wait_recv()
            arrived = rs_in[layer, src].astype(F32)
            own_part[x, : 6 * rows] += arrived[: 6 * rows]
            own_part[x, 6 * rows : 6 * rows + 8] += arrived[6 * rows : 6 * rows + 8] + arrived[6 * rows + 8 :]

        by_distance(n_x, add_sums)

        squares = own_part[x, 6 * rows : 6 * rows + 8]
        inv = lax.rsqrt(squares / model + norm_epsilon)
        inv_rows = jnp.concatenate(
            [jnp.broadcast_to(inv[:, 32 * g : 32 * g + 1], (8, LANES)) for g in range(rows // 8)], 0
        )
        recept, keys, values, decay_pre, rate_pre, gate_pre = [
            (inv_rows * own_part[x, i * rows : (i + 1) * rows]).astype(BF16).astype(F32) for i in range(6)
        ]
        raw = base_ref[pl.ds(layer, 1), :] + decay_pre
        decays = jnp.exp(-jnp.exp(jnp.float32(-0.5)) / (1.0 + jnp.exp(-raw)))
        rates = 1.0 / (1.0 + jnp.exp(-rate_pre))
        unit = keys * lax.rsqrt(dot_split(keys * keys, same_half) + unit_epsilon)
        zero = jnp.zeros_like(keys)
        decays = jnp.where(live, decays, 1.0)
        drop = jnp.where(live, unit * rates, zero)
        put = jnp.where(live, keys, zero)

        def tile_maker(q):
            turned = pltpu.roll(q, HEAD, 1)

            def tiles(n):
                made = []
                for s in range(seqs):
                    at = NEW * s + n
                    made.append(
                        jnp.where(
                            m8,
                            jnp.broadcast_to(q[at : at + 1], (8, LANES)),
                            jnp.broadcast_to(turned[at : at + 1], (8, LANES)),
                        )
                    )
                return jnp.stack(made)[:, None]

            return tiles

        decay_tiles, unit_tiles, drop_tiles, put_tiles, recept_tiles = [
            tile_maker(q) for q in (decays, unit, drop, put, recept)
        ]
        full = (seqs, 8, 8, LANES)
        flat = (seqs * HEAD, LANES)
        memory = st_v[layer].reshape(full)
        reads = jnp.zeros((rows, LANES), F32)
        for n in range(NEW):
            value_rows = jnp.stack(
                [jnp.broadcast_to(values[NEW * s + n : NEW * s + n + 1], (8, LANES)) for s in range(seqs)]
            )[:, None]
            value_full = dot((value_rows * entry).reshape(flat).astype(BF16), spread).reshape(full)
            removed = dot_split((memory * unit_tiles(n)).reshape(flat), same_half).reshape(full)
            memory = memory * decay_tiles(n) - removed * drop_tiles(n) + value_full * put_tiles(n)
            seen = dot_split((memory * recept_tiles(n)).reshape(flat), collect).reshape(full)
            seen = jnp.sum(seen * entry, axis=1).reshape(seqs * 8, LANES)
            pick_shape = (rows, seqs * 8)
            pick = (iota(pick_shape, 0) == (iota(pick_shape, 1) // 8) * NEW + n).astype(F32).astype(BF16)
            seen_high = seen.astype(BF16)
            seen_low = (seen - seen_high.astype(F32)).astype(BF16)
            reads = reads + dot(pick, seen_high) + dot(pick, seen_low)
        st_v[layer] = memory.reshape(flat)
        pltpu.make_async_copy(st_v.at[layer], states_out.at[layer], st_sem.at[layer]).start()

        mean = dot_split(reads, same_half) / HEAD
        dev = reads - mean
        var = dot_split(dev * dev, same_half) / HEAD
        normed = dev * lax.rsqrt(var + group_epsilon) * group_ref[pl.ds(layer, 1), :]
        mixed = jnp.where(live, normed / (1.0 + jnp.exp(-gate_pre)), zero)
        mix_buf[layer, d] = mixed.astype(BF16)

        def send_mixed(off):
            d_copy(layer, lax.rem(d + off, n_dp), d).start()

        by_distance(n_dp, send_mixed)
        for j in far_first:
            blocks = [around(off + 4 * j) for off in targets + (0,)]
            for block in blocks:
                @pl.when(block != d)
                def _():
                    d_copy(layer, d, block).wait_recv()

            partial = dot(jnp.concatenate([mix_buf[layer, block] for block in blocks], 0), wo_v[layer])
            partial = partial.reshape(4, rows, feats)
            for i, off in enumerate(targets):
                part_out[layer, blocks[i]] = partial[i].astype(BF16)
                near_copy(layer, j, i, blocks[i], around(off)).start()
            class_sum[j] = partial[3]
        for j in far_first:
            total = class_sum[j]
            for i in range(3):
                near_copy(layer, j, i, t, t).wait_recv()
                total = total + part_in[layer, 3 * j + i].astype(F32)
            if j:
                far_out[layer, j] = total.astype(BF16)
                far_copy(layer, j, around(4 * j)).start()
            else:
                own_rows = own_rows + total
        for j in near_first[1:]:
            far_copy(layer, j, t).wait_recv()
            own_rows = own_rows + far_in[layer, j].astype(F32)
        own_rows = own_rows.astype(BF16)
        if layer == 0:
            x_buf[1, t] = own_rows
            gather_start(1, x_buf.at[1, t])
            own_rows = own_rows.astype(F32)
        else:
            tokens_out[...] = own_rows

    for layer in range(2):
        for k in range(n_tp - 1):
            g_copy(layer, tokens_ref, t, t, k).wait_send()
        for j in range(hops):
            for i in range(3):
                near_copy(layer, j, i, t, t).wait_send()
            if j:
                far_copy(layer, j, t).wait_send()

        def drain_d(off):
            d_copy(layer, lax.rem(d + off, n_dp), d).wait_send()

        def drain_rs(off):
            place = lax.rem(x + off, n_x)
            rs_copy(layer, place, x).wait_send()
            pair_copy(layer, place).wait_send()

        by_distance(n_dp, drain_d)
        by_distance(n_x, drain_rs)
        pair_copy(layer, x).wait_send()
        pltpu.make_async_copy(st_v.at[layer], states_out.at[layer], st_sem.at[layer]).wait()


def per_device(n_tp, n_dp, tokens, lengths, norm_gain, w_recept, w_keys, w_values, w_decay, w_rate, w_gate,
               decay_base, group_gain, w_out, states):
    rows, feats = tokens.shape
    layers, seqs, heads, flat = states.shape
    folded = flat // LANES
    width = w_recept.shape[2]
    n_x = n_dp // 2
    state_rows = seqs * folded * heads
    packed = states.reshape(layers, seqs, heads, folded, LANES).transpose(0, 1, 3, 2, 4)
    packed = packed.reshape(layers, state_rows, LANES)
    vmem = pl.BlockSpec(memory_space=pltpu.VMEM)
    hbm = pl.BlockSpec(memory_space=pltpu.HBM)
    msg = 6 * rows + 16
    out, new_states = pl.pallas_call(
        functools.partial(kernel, n_tp, n_dp),
        out_shape=(
            jax.ShapeDtypeStruct((rows, feats), BF16),
            jax.ShapeDtypeStruct((layers, state_rows, LANES), F32),
        ),
        in_specs=[hbm] * 13,
        out_specs=(vmem, hbm),
        scratch_shapes=[
            pltpu.VMEM((rows, feats), BF16),
            pltpu.SMEM((seqs,), jnp.int32),
            pltpu.VMEM((layers, feats), F32),
            pltpu.VMEM((layers, width), F32),
            pltpu.VMEM((layers, width), F32),
            pltpu.VMEM((layers, feats, 6 * width), BF16),
            pltpu.VMEM((layers, width, feats), BF16),
            pltpu.VMEM((layers, state_rows, LANES), F32),
            pltpu.VMEM((layers, n_tp, rows, feats), BF16),
            pltpu.VMEM((layers, n_x, msg, width), BF16),
            pltpu.VMEM((layers, n_x, msg, width), BF16),
            pltpu.VMEM((n_x, msg, width), F32),
            pltpu.VMEM((layers, n_x, msg, width), BF16),
            pltpu.VMEM((layers, n_x, msg, width), BF16),
            pltpu.VMEM((layers, n_dp, rows, width), BF16),
            pltpu.VMEM((layers, n_tp, rows, feats), BF16),
            pltpu.VMEM((layers, 3 * n_tp // 4, rows, feats), BF16),
            pltpu.VMEM((n_tp // 4, rows, feats), F32),
            pltpu.VMEM((layers, n_tp // 4, rows, feats), BF16),
            pltpu.VMEM((layers, n_tp // 4, rows, feats), BF16),
            pltpu.SemaphoreType.DMA((13,)),
            pltpu.SemaphoreType.DMA((2,)),
            pltpu.SemaphoreType.DMA((2, n_tp)),
            pltpu.SemaphoreType.DMA((2, n_tp)),
            pltpu.SemaphoreType.DMA((2, n_tp)),
            pltpu.SemaphoreType.DMA((2, n_tp)),
            pltpu.SemaphoreType.DMA((2, n_dp)),
            pltpu.SemaphoreType.DMA((2, n_dp)),
            pltpu.SemaphoreType.DMA((2, n_x)),
            pltpu.SemaphoreType.DMA((2, n_x)),
            pltpu.SemaphoreType.DMA((2, n_x)),
            pltpu.SemaphoreType.DMA((2, n_x)),
        ],
        compiler_params=pltpu.CompilerParams(
            collective_id=0, has_side_effects=True, vmem_limit_bytes=67043328
        ),
    )(tokens, lengths, norm_gain, decay_base, group_gain,
      w_recept, w_keys, w_values, w_decay, w_rate, w_gate, w_out, packed)
    new_states = new_states.reshape(layers, seqs, folded, heads, LANES).transpose(0, 1, 3, 2, 4)
    return out, new_states.reshape(layers, seqs, heads, flat)


def solution(mesh):
    placed = (
        P(("grp", "tp"), "dp"),
        P(("grp", "dp")),
        P(None, "dp"),
        P(None, "dp", "tp"),
        P(None, "dp", "tp"),
        P(None, "dp", "tp"),
        P(None, "dp", "tp"),
        P(None, "dp", "tp"),
        P(None, "dp", "tp"),
        P(None, "tp"),
        P(None, "tp"),
        P(None, "tp", "dp"),
        P(None, ("grp", "dp"), "tp", None),
    )
    return jax.shard_map(
        functools.partial(per_device, mesh.shape["tp"], mesh.shape["dp"]),
        mesh=mesh,
        in_specs=placed,
        out_specs=(P(("grp", "tp"), "dp"), P(None, ("grp", "dp"), "tp", None)),
        check_vma=False,
    )
```

```python
import functools

import jax
import jax.numpy as jnp
from jax import lax
from jax.experimental import pallas as pl
from jax.experimental.pallas import tpu as pltpu
from jax.sharding import PartitionSpec as P

HEAD = 64
NEW = 4
LANES = 128
HALVES = 2
norm_epsilon = 1e-06
unit_epsilon = 0.00064
group_epsilon = 0.00064
MESH = pl.DeviceIdType.MESH
F32 = jnp.float32
BF16 = jnp.bfloat16


def iota(shape, dim):
    return lax.broadcasted_iota(jnp.int32, shape, dim)


def dot(a, b):
    return jnp.dot(a, b, preferred_element_type=F32)


def dot_split(a, b):
    high = a.astype(BF16)
    low = (a - high.astype(F32)).astype(BF16)
    return dot(high, b) + dot(low, b)


def pair_rows(value):
    high = value.astype(BF16).astype(F32)
    return jnp.concatenate([high, value - high], axis=-2)


def by_distance(n, act):
    act(n // 2)

    def body(step, carry):
        dist = n // 2 - 1 - step
        act(dist)
        act(n - dist)
        return carry

    lax.fori_loop(0, n // 2 - 1, body, 0)


def kernel(
    n_tp, n_dp,
    tokens_hbm, lengths_hbm, gain_hbm, base_hbm, group_hbm,
    w0, w1, w2, w3, w4, w5, wout_hbm, states_hbm,
    tokens_out, states_out,
    tokens_ref, lengths_ref, gain_ref, base_ref, group_ref,
    w_v, wo_v, st_v, x_buf, pair_out, pair_in, own_part, rs_out, rs_in, mix_buf,
    part_out, part_in, class_sum, far_out, far_in,
    local_sem, g_send, g_recv, p_send, p_recv, d_send, d_recv, rs_send, rs_recv, pair_send, pair_recv,
):
    t = lax.axis_index("tp")
    d = lax.axis_index("dp")
    n_x = n_dp // 2
    x = d // 2
    c = d % 2
    _, rows, feats = tokens_ref.shape
    seqs = rows // NEW
    width = LANES
    model = feats * n_dp
    hops = n_tp // 4
    near_first = sorted(range(hops), key=lambda j: min(j, hops - j))
    far_first = near_first[::-1]

    first = [
        pltpu.make_async_copy(tokens_hbm.at[pl.ds(h * rows, rows)], tokens_ref.at[h], local_sem.at[8 + 5 * h])
        for h in range(HALVES)
    ]
    for load in first:
        load.start()
    loads = [
        pltpu.make_async_copy(gain_hbm, gain_ref, local_sem.at[9]),
        pltpu.make_async_copy(base_hbm, base_ref, local_sem.at[10]),
        pltpu.make_async_copy(group_hbm, group_ref, local_sem.at[11]),
        pltpu.make_async_copy(lengths_hbm, lengths_ref, local_sem.at[12]),
    ]
    for i, w in enumerate((w0, w1, w2, w3, w4, w5)):
        loads.append(
            pltpu.make_async_copy(w, w_v.at[:, :, pl.ds(i * width, width)], local_sem.at[i])
        )
    loads.append(pltpu.make_async_copy(wout_hbm, wo_v, local_sem.at[6]))
    loads.append(pltpu.make_async_copy(states_hbm, st_v, local_sem.at[7]))
    for load in loads:
        load.start()

    def around(off):
        return lax.rem(t + off + 2 * n_tp, n_tp)

    skip = 2 - 4 * (t % 2)
    targets = (1, -1, skip)
    sources = (-1, 1, -skip)

    barrier = pltpu.get_barrier_semaphore()

    def greet_z(off):
        pl.semaphore_signal(barrier, inc=1, device_id={"tp": around(off)}, device_id_type=MESH)

    def greet_d(off):
        pl.semaphore_signal(barrier, inc=1, device_id={"dp": lax.rem(d + off, n_dp)}, device_id_type=MESH)

    for j in far_first:
        if j:
            greet_z(4 * j)
    for off in targets + sources[2:]:
        greet_z(off)
    by_distance(n_dp, greet_d)
    for load in first:
        load.wait()
    pl.semaphore_wait(barrier, (hops - 1) + 4 + n_dp - 1)

    def g_copy(chain, src, block, peer, k):
        return pltpu.make_async_remote_copy(
            src_ref=src, dst_ref=x_buf.at[chain, block],
            send_sem=g_send.at[chain, k], recv_sem=g_recv.at[chain, block],
            device_id={"tp": peer}, device_id_type=MESH,
        )

    def near_copy(chain, j, i, block, peer):
        return pltpu.make_async_remote_copy(
            src_ref=part_out.at[chain, block], dst_ref=part_in.at[chain, 3 * j + i],
            send_sem=p_send.at[chain, 3 * j + i], recv_sem=p_recv.at[chain, 3 * j + i],
            device_id={"tp": peer}, device_id_type=MESH,
        )

    def far_copy(chain, j, peer):
        return pltpu.make_async_remote_copy(
            src_ref=far_out.at[chain, j], dst_ref=far_in.at[chain, j],
            send_sem=p_send.at[chain, 3 * hops + j - 1], recv_sem=p_recv.at[chain, 3 * hops + j - 1],
            device_id={"tp": peer}, device_id_type=MESH,
        )

    def d_copy(chain, peer, slot):
        return pltpu.make_async_remote_copy(
            src_ref=mix_buf.at[chain, d], dst_ref=mix_buf.at[chain, slot],
            send_sem=d_send.at[chain, peer], recv_sem=d_recv.at[chain, slot],
            device_id={"dp": peer}, device_id_type=MESH,
        )

    def rs_copy(chain, peer, slot):
        return pltpu.make_async_remote_copy(
            src_ref=rs_out.at[chain, peer], dst_ref=rs_in.at[chain, slot],
            send_sem=rs_send.at[chain, peer], recv_sem=rs_recv.at[chain, slot],
            device_id={"dp": peer * 2 + c}, device_id_type=MESH,
        )

    def pair_copy(chain, place):
        return pltpu.make_async_remote_copy(
            src_ref=pair_out.at[chain, place], dst_ref=pair_in.at[chain, place],
            send_sem=pair_send.at[chain, place], recv_sem=pair_recv.at[chain, place],
            device_id={"dp": x * 2 + (1 - c)}, device_id_type=MESH,
        )

    def gather_start(chain, src):
        for j in far_first:
            if j:
                g_copy(chain, src, t, around(4 * j), 3 * hops + j - 1).start()
        for i, off in enumerate(targets):
            g_copy(chain, src, t, around(off), i).start()

    def gather_forward(chain, j):
        block = around(4 * j)
        g_copy(chain, x_buf.at[chain, block], block, t, 0).wait_recv()
        for i, off in enumerate(targets):
            g_copy(chain, x_buf.at[chain, block], block, around(off), 3 * j + i).start()

    def gather_near(chain, j):
        for off in sources:
            block = around(off + 4 * j)
            g_copy(chain, x_buf.at[chain, block], block, t, 0).wait_recv()

    for h in range(HALVES):
        gather_start(h, tokens_ref.at[h])
    for h in range(HALVES):
        x_buf[h, t] = tokens_ref[h]
    own_rows = [tokens_ref[h].astype(F32) for h in range(HALVES)]
    for load in loads:
        load.wait()

    lane8 = iota((8, LANES), 1)
    m8 = (lane8 // HEAD) == (iota((8, LANES), 0) % 2)
    sq = (LANES, LANES)
    same_half = ((iota(sq, 0) // HEAD) == (iota(sq, 1) // HEAD)).astype(F32).astype(BF16)
    spread = ((iota(sq, 0) % 2) == (iota(sq, 1) // HEAD)).astype(F32).astype(BF16)
    collect = ((iota(sq, 0) // HEAD) == (iota(sq, 1) % 2)).astype(F32).astype(BF16)
    tall = (HEAD, LANES)
    row_of = iota(tall, 0)
    lane_of = iota(tall, 1)
    entry = (((lane_of // HEAD) == (row_of % 2)) & (((lane_of % HEAD) // 2) == (row_of // 2))).astype(F32)
    entry = entry.reshape(1, 8, 8, LANES)
    tok_row = iota((rows, LANES), 0)
    live_rows = []
    for h in range(HALVES):
        length_rows = jnp.zeros((rows, LANES), jnp.int32)
        for q in range(seqs):
            length_rows = jnp.where((tok_row // NEW) == q, lengths_ref[h * seqs + q], length_rows)
        live_rows.append((tok_row % NEW) < length_rows)
    groups = rows // 8
    span = LANES // groups

    odd = (t + c) % 2
    even = 1 - odd
    mine = (-odd, odd - even * skip)
    theirs = (-even, even - odd * skip)

    def wave(layer, h, j):
        chain = HALVES * layer + h
        blocks = [around(off + 4 * j) for off in theirs + mine]
        wide = jnp.concatenate([x_buf[chain, block] for block in blocks], 0).astype(F32)
        total = jnp.sum(wide * wide, axis=-1, keepdims=True)
        total = jnp.broadcast_to(total, (4 * rows, LANES)).reshape(4, groups, 8, LANES)
        packed = total[:, 0]
        for g in range(1, groups):
            packed = jnp.where(lane8 // span == g, total[:, g], packed)
        scaled = (wide * gain_ref[pl.ds(layer, 1), :]).astype(BF16)
        for p in range(3):
            out = dot(scaled, w_v[layer, :, 2 * width * p : 2 * width * (p + 1)])
            for k in range(2):
                i = 2 * p + k
                piece = out[:, k * width : (k + 1) * width].reshape(4, rows, width)
                for q in range(2):
                    pair_out[chain, blocks[q] // 2, i * rows : (i + 1) * rows] = piece[q].astype(BF16)
                    own_part[h, blocks[2 + q] // 2, i * rows : (i + 1) * rows] = piece[2 + q]
        for q in range(2):
            pair_out[chain, blocks[q] // 2, 6 * rows :] = pair_rows(packed[q]).astype(BF16)
            own_part[h, blocks[2 + q] // 2, 6 * rows : 6 * rows + 8] = packed[2 + q]
        for q in range(2):
            pair_copy(chain, blocks[q] // 2).start()

    def both(chain, h, place):
        arrived = pair_in[chain, place].astype(F32)
        main = own_part[h, place, : 6 * rows] + arrived[: 6 * rows]
        squares = own_part[h, place, 6 * rows : 6 * rows + 8] + (
            arrived[6 * rows : 6 * rows + 8] + arrived[6 * rows + 8 :]
        )
        return main, squares

    def finish(layer, h, j):
        chain = HALVES * layer + h
        for off in mine:
            place = around(off + 4 * j) // 2
            pair_copy(chain, place).wait_recv()
            main, squares = both(chain, h, place)

            @pl.when(place != x)
            def _():
                rs_out[chain, place, : 6 * rows] = main.astype(BF16)
                rs_out[chain, place, 6 * rows :] = pair_rows(squares).astype(BF16)
                rs_copy(chain, place, x).start()

            @pl.when(place == x)
            def _():
                own_part[h, x, : 6 * rows] = main
                own_part[h, x, 6 * rows : 6 * rows + 8] = squares

    def sum_and_advance(layer, h):
        chain = HALVES * layer + h

        def add_sums(off):
            src = lax.rem(x + off, n_x)
            rs_copy(chain, x, src).wait_recv()
            arrived = rs_in[chain, src].astype(F32)
            own_part[h, x, : 6 * rows] += arrived[: 6 * rows]
            own_part[h, x, 6 * rows : 6 * rows + 8] += arrived[6 * rows : 6 * rows + 8] + arrived[6 * rows + 8 :]

        by_distance(n_x, add_sums)

        squares = own_part[h, x, 6 * rows : 6 * rows + 8]
        inv = lax.rsqrt(squares / model + norm_epsilon)
        inv_rows = jnp.concatenate(
            [jnp.broadcast_to(inv[:, span * g : span * g + 1], (8, LANES)) for g in range(groups)], 0
        )
        recept, keys, values, decay_pre, rate_pre, gate_pre = [
            (inv_rows * own_part[h, x, i * rows : (i + 1) * rows]).astype(BF16).astype(F32) for i in range(6)
        ]
        raw = base_ref[pl.ds(layer, 1), :] + decay_pre
        decays = jnp.exp(-jnp.exp(jnp.float32(-0.5)) / (1.0 + jnp.exp(-raw)))
        rates = 1.0 / (1.0 + jnp.exp(-rate_pre))
        unit = keys * lax.rsqrt(dot_split(keys * keys, same_half) + unit_epsilon)
        zero = jnp.zeros_like(keys)
        decays = jnp.where(live_rows[h], decays, 1.0)
        drop = jnp.where(live_rows[h], unit * rates, zero)
        put = jnp.where(live_rows[h], keys, zero)

        def tile_maker(q):
            turned = pltpu.roll(q, HEAD, 1)

            def tiles(n):
                made = []
                for s in range(seqs):
                    at = NEW * s + n
                    made.append(
                        jnp.where(
                            m8,
                            jnp.broadcast_to(q[at : at + 1], (8, LANES)),
                            jnp.broadcast_to(turned[at : at + 1], (8, LANES)),
                        )
                    )
                return jnp.stack(made)[:, None]

            return tiles

        decay_tiles, unit_tiles, drop_tiles, put_tiles, recept_tiles = [
            tile_maker(q) for q in (decays, unit, drop, put, recept)
        ]
        full = (seqs, 8, 8, LANES)
        flat = (seqs * HEAD, LANES)
        memory = st_v[layer, pl.ds(h * seqs * HEAD, seqs * HEAD)].reshape(full)
        reads = jnp.zeros((rows, LANES), F32)
        for n in range(NEW):
            value_rows = jnp.stack(
                [jnp.broadcast_to(values[NEW * s + n : NEW * s + n + 1], (8, LANES)) for s in range(seqs)]
            )[:, None]
            value_full = dot((value_rows * entry).reshape(flat).astype(BF16), spread).reshape(full)
            removed = dot_split((memory * unit_tiles(n)).reshape(flat), same_half).reshape(full)
            memory = memory * decay_tiles(n) - removed * drop_tiles(n) + value_full * put_tiles(n)
            seen = dot_split((memory * recept_tiles(n)).reshape(flat), collect).reshape(full)
            seen = jnp.sum(seen * entry, axis=1).reshape(seqs * 8, LANES)
            pick_shape = (rows, seqs * 8)
            pick = (iota(pick_shape, 0) == (iota(pick_shape, 1) // 8) * NEW + n).astype(F32).astype(BF16)
            seen_high = seen.astype(BF16)
            seen_low = (seen - seen_high.astype(F32)).astype(BF16)
            reads = reads + dot(pick, seen_high) + dot(pick, seen_low)
        states_out[layer, pl.ds(h * seqs * HEAD, seqs * HEAD)] = memory.reshape(flat)

        mean = dot_split(reads, same_half) / HEAD
        dev = reads - mean
        var = dot_split(dev * dev, same_half) / HEAD
        normed = dev * lax.rsqrt(var + group_epsilon) * group_ref[pl.ds(layer, 1), :]
        mixed = jnp.where(live_rows[h], normed / (1.0 + jnp.exp(-gate_pre)), zero)
        mix_buf[chain, d] = mixed.astype(BF16)

        def send_mixed(off):
            d_copy(chain, lax.rem(d + off, n_dp), d).start()

        by_distance(n_dp, send_mixed)

    def project_out(layer, h):
        chain = HALVES * layer + h
        for j in far_first:
            blocks = [around(off + 4 * j) for off in targets + (0,)]
            for block in blocks:
                @pl.when(block != d)
                def _():
                    d_copy(chain, d, block).wait_recv()

            partial = dot(jnp.concatenate([mix_buf[chain, block] for block in blocks], 0), wo_v[layer])
            partial = partial.reshape(4, rows, feats)
            for i, off in enumerate(targets):
                part_out[chain, blocks[i]] = partial[i].astype(BF16)
                near_copy(chain, j, i, blocks[i], around(off)).start()
            class_sum[h, j] = partial[3]

    def sum_classes(layer, h):
        chain = HALVES * layer + h
        for j in far_first:
            total = class_sum[h, j]
            for i in range(3):
                near_copy(chain, j, i, t, t).wait_recv()
                total = total + part_in[chain, 3 * j + i].astype(F32)
            if j:
                far_out[chain, j] = total.astype(BF16)
                far_copy(chain, j, around(4 * j)).start()
            else:
                own_rows[h] = own_rows[h] + total

    def end_block(layer, h):
        chain = HALVES * layer + h
        for j in near_first[1:]:
            far_copy(chain, j, t).wait_recv()
            own_rows[h] = own_rows[h] + far_in[chain, j].astype(F32)
        done = own_rows[h].astype(BF16)
        if layer == 0:
            x_buf[HALVES + h, t] = done
            gather_start(HALVES + h, x_buf.at[HALVES + h, t])
            own_rows[h] = done.astype(F32)
        else:
            tokens_out[pl.ds(h * rows, rows)] = done

    middle, last = near_first[1:-1], near_first[1:][-1:]
    halves = range(HALVES)
    for layer in range(2):
        chains = [HALVES * layer + h for h in halves]
        for h in halves:
            gather_near(chains[h], 0)
            wave(layer, h, 0)
            for j in middle:
                gather_forward(chains[h], j)
        for h in halves:
            finish(layer, h, 0)
        for j in last:
            for h in halves:
                gather_forward(chains[h], j)
        for h in halves:
            for j in middle:
                gather_near(chains[h], j)
                wave(layer, h, j)
        for h in halves:
            for j in middle:
                finish(layer, h, j)
        for j in last:
            for h in halves:
                gather_near(chains[h], j)
                wave(layer, h, j)
            for h in halves:
                finish(layer, h, j)
        for stage in (sum_and_advance, project_out, sum_classes, end_block):
            for h in halves:
                stage(layer, h)

    for chain in range(2 * HALVES):
        for k in range(n_tp - 1):
            g_copy(chain, tokens_ref.at[0], t, t, k).wait_send()
        for j in range(hops):
            for i in range(3):
                near_copy(chain, j, i, t, t).wait_send()
            if j:
                far_copy(chain, j, t).wait_send()

        def drain_d(off):
            d_copy(chain, lax.rem(d + off, n_dp), d).wait_send()

        def drain_rs(off):
            place = lax.rem(x + off, n_x)
            rs_copy(chain, place, x).wait_send()
            pair_copy(chain, place).wait_send()

        by_distance(n_dp, drain_d)
        by_distance(n_x, drain_rs)
        pair_copy(chain, x).wait_send()


def per_device(n_tp, n_dp, tokens, lengths, norm_gain, w_recept, w_keys, w_values, w_decay, w_rate, w_gate,
               decay_base, group_gain, w_out, states):
    rows, feats = tokens.shape
    layers, seqs, heads, flat = states.shape
    folded = flat // LANES
    width = w_recept.shape[2]
    n_x = n_dp // 2
    state_rows = seqs * folded * heads
    packed = states.reshape(layers, seqs, heads, folded, LANES).transpose(0, 1, 3, 2, 4)
    packed = packed.reshape(layers, state_rows, LANES)
    vmem = pl.BlockSpec(memory_space=pltpu.VMEM)
    hbm = pl.BlockSpec(memory_space=pltpu.HBM)
    part = rows // HALVES
    chains = layers * HALVES
    msg = 6 * part + 16
    out, new_states = pl.pallas_call(
        functools.partial(kernel, n_tp, n_dp),
        out_shape=(
            jax.ShapeDtypeStruct((rows, feats), BF16),
            jax.ShapeDtypeStruct((layers, state_rows, LANES), F32),
        ),
        in_specs=[hbm] * 13,
        out_specs=(vmem, vmem),
        scratch_shapes=[
            pltpu.VMEM((HALVES, part, feats), BF16),
            pltpu.SMEM((seqs,), jnp.int32),
            pltpu.VMEM((layers, feats), F32),
            pltpu.VMEM((layers, width), F32),
            pltpu.VMEM((layers, width), F32),
            pltpu.VMEM((layers, feats, 6 * width), BF16),
            pltpu.VMEM((layers, width, feats), BF16),
            pltpu.VMEM((layers, state_rows, LANES), F32),
            pltpu.VMEM((chains, n_tp, part, feats), BF16),
            pltpu.VMEM((chains, n_x, msg, width), BF16),
            pltpu.VMEM((chains, n_x, msg, width), BF16),
            pltpu.VMEM((HALVES, n_x, msg, width), F32),
            pltpu.VMEM((chains, n_x, msg, width), BF16),
            pltpu.VMEM((chains, n_x, msg, width), BF16),
            pltpu.VMEM((chains, n_dp, part, width), BF16),
            pltpu.VMEM((chains, n_tp, part, feats), BF16),
            pltpu.VMEM((chains, 3 * n_tp // 4, part, feats), BF16),
            pltpu.VMEM((HALVES, n_tp // 4, part, feats), F32),
            pltpu.VMEM((chains, n_tp // 4, part, feats), BF16),
            pltpu.VMEM((chains, n_tp // 4, part, feats), BF16),
            pltpu.SemaphoreType.DMA((14,)),
        ] + [pltpu.SemaphoreType.DMA((chains, n_tp))] * 4
        + [pltpu.SemaphoreType.DMA((chains, n_dp))] * 2
        + [pltpu.SemaphoreType.DMA((chains, n_x))] * 4,
        compiler_params=pltpu.CompilerParams(
            collective_id=0, has_side_effects=True, vmem_limit_bytes=48 * 1024 * 1024
        ),
    )(*[
        pltpu.with_memory_space_constraint(operand, pltpu.HBM)
        for operand in (tokens, lengths, norm_gain, decay_base, group_gain,
                        w_recept, w_keys, w_values, w_decay, w_rate, w_gate, w_out, packed)
    ])
    new_states = new_states.reshape(layers, seqs, folded, heads, LANES).transpose(0, 1, 3, 2, 4)
    return out, new_states.reshape(layers, seqs, heads, flat)


def solution(mesh):
    placed = (
        P(("grp", "tp"), "dp"),
        P(("grp", "dp")),
        P(None, "dp"),
        P(None, "dp", "tp"),
        P(None, "dp", "tp"),
        P(None, "dp", "tp"),
        P(None, "dp", "tp"),
        P(None, "dp", "tp"),
        P(None, "dp", "tp"),
        P(None, "tp"),
        P(None, "tp"),
        P(None, "tp", "dp"),
        P(None, ("grp", "dp"), "tp", None),
    )
    return jax.shard_map(
        functools.partial(per_device, mesh.shape["tp"], mesh.shape["dp"]),
        mesh=mesh,
        in_specs=placed,
        out_specs=(P(("grp", "tp"), "dp"), P(None, ("grp", "dp"), "tp", None)),
        check_vma=False,
    )
```

```python
import functools

import jax
import jax.numpy as jnp
from jax import lax
from jax.experimental import pallas as pl
from jax.experimental.pallas import tpu as pltpu
from jax.sharding import PartitionSpec as P

HEAD = 64
NEW = 4
LANES = 128
HALVES = 1
norm_epsilon = 1e-06
unit_epsilon = 0.00064
group_epsilon = 0.00064
MESH = pl.DeviceIdType.MESH
F32 = jnp.float32
BF16 = jnp.bfloat16


def iota(shape, dim):
    return lax.broadcasted_iota(jnp.int32, shape, dim)


def dot(a, b):
    return jnp.dot(a, b, preferred_element_type=F32)


def dot_split(a, b):
    high = a.astype(BF16)
    low = (a - high.astype(F32)).astype(BF16)
    return dot(high, b) + dot(low, b)


def pair_rows(value):
    high = value.astype(BF16).astype(F32)
    return jnp.concatenate([high, value - high], axis=-2)


def by_distance(n, act):
    act(n // 2)

    def body(step, carry):
        dist = n // 2 - 1 - step
        act(dist)
        act(n - dist)
        return carry

    lax.fori_loop(0, n // 2 - 1, body, 0)


def kernel(
    n_tp, n_dp,
    tokens_hbm, lengths_hbm, gain_hbm, base_hbm, group_hbm,
    w0, w1, w2, w3, w4, w5, wout_hbm, states_hbm,
    tokens_out, states_out,
    tokens_ref, lengths_ref, gain_ref, base_ref, group_ref,
    w_v, wo_v, st_v, x_buf, pair_out, pair_in, own_part, rs_out, rs_in, mix_buf,
    part_out, part_in, class_sum, far_out, far_in,
    local_sem, g_send, g_recv, p_send, p_recv, d_send, d_recv, rs_send, rs_recv, pair_send, pair_recv,
):
    t = lax.axis_index("tp")
    d = lax.axis_index("dp")
    n_x = n_dp // 2
    x = d // 2
    c = d % 2
    _, rows, feats = tokens_ref.shape
    seqs = rows // NEW
    width = LANES
    model = feats * n_dp
    hops = n_tp // 4
    near_first = sorted(range(hops), key=lambda j: min(j, hops - j))
    far_first = near_first[::-1]

    first = [
        pltpu.make_async_copy(tokens_hbm.at[pl.ds(h * rows, rows)], tokens_ref.at[h], local_sem.at[8 + 5 * h])
        for h in range(HALVES)
    ]
    for load in first:
        load.start()
    loads = [
        pltpu.make_async_copy(gain_hbm, gain_ref, local_sem.at[9]),
        pltpu.make_async_copy(base_hbm, base_ref, local_sem.at[10]),
        pltpu.make_async_copy(group_hbm, group_ref, local_sem.at[11]),
        pltpu.make_async_copy(lengths_hbm, lengths_ref, local_sem.at[12]),
    ]
    for i, w in enumerate((w0, w1, w2, w3, w4, w5)):
        loads.append(
            pltpu.make_async_copy(w, w_v.at[:, :, pl.ds(i * width, width)], local_sem.at[i])
        )
    loads.append(pltpu.make_async_copy(wout_hbm, wo_v, local_sem.at[6]))
    loads.append(pltpu.make_async_copy(states_hbm, st_v, local_sem.at[7]))
    for load in loads:
        load.start()

    def around(off):
        return lax.rem(t + off + 2 * n_tp, n_tp)

    skip = 2 - 4 * (t % 2)
    targets = (1, -1, skip)
    sources = (-1, 1, -skip)

    barrier = pltpu.get_barrier_semaphore()

    def greet_z(off):
        pl.semaphore_signal(barrier, inc=1, device_id={"tp": around(off)}, device_id_type=MESH)

    def greet_d(off):
        pl.semaphore_signal(barrier, inc=1, device_id={"dp": lax.rem(d + off, n_dp)}, device_id_type=MESH)

    for j in far_first:
        if j:
            greet_z(4 * j)
    for off in targets + sources[2:]:
        greet_z(off)
    by_distance(n_dp, greet_d)
    for load in first:
        load.wait()
    pl.semaphore_wait(barrier, (hops - 1) + 4 + n_dp - 1)

    def g_copy(chain, src, block, peer, k):
        return pltpu.make_async_remote_copy(
            src_ref=src, dst_ref=x_buf.at[chain, block],
            send_sem=g_send.at[chain, k], recv_sem=g_recv.at[chain, block],
            device_id={"tp": peer}, device_id_type=MESH,
        )

    def near_copy(chain, j, i, block, peer):
        return pltpu.make_async_remote_copy(
            src_ref=part_out.at[chain, block], dst_ref=part_in.at[chain, 3 * j + i],
            send_sem=p_send.at[chain, 3 * j + i], recv_sem=p_recv.at[chain, 3 * j + i],
            device_id={"tp": peer}, device_id_type=MESH,
        )

    def far_copy(chain, j, peer):
        return pltpu.make_async_remote_copy(
            src_ref=far_out.at[chain, j], dst_ref=far_in.at[chain, j],
            send_sem=p_send.at[chain, 3 * hops + j - 1], recv_sem=p_recv.at[chain, 3 * hops + j - 1],
            device_id={"tp": peer}, device_id_type=MESH,
        )

    def d_copy(chain, peer, slot):
        return pltpu.make_async_remote_copy(
            src_ref=mix_buf.at[chain, d], dst_ref=mix_buf.at[chain, slot],
            send_sem=d_send.at[chain, peer], recv_sem=d_recv.at[chain, slot],
            device_id={"dp": peer}, device_id_type=MESH,
        )

    def rs_copy(chain, peer, slot):
        return pltpu.make_async_remote_copy(
            src_ref=rs_out.at[chain, peer], dst_ref=rs_in.at[chain, slot],
            send_sem=rs_send.at[chain, peer], recv_sem=rs_recv.at[chain, slot],
            device_id={"dp": peer * 2 + c}, device_id_type=MESH,
        )

    def pair_copy(chain, place):
        return pltpu.make_async_remote_copy(
            src_ref=pair_out.at[chain, place], dst_ref=pair_in.at[chain, place],
            send_sem=pair_send.at[chain, place], recv_sem=pair_recv.at[chain, place],
            device_id={"dp": x * 2 + (1 - c)}, device_id_type=MESH,
        )

    def gather_start(chain, src):
        for j in far_first:
            if j:
                g_copy(chain, src, t, around(4 * j), 3 * hops + j - 1).start()
        for i, off in enumerate(targets):
            g_copy(chain, src, t, around(off), i).start()

    def gather_forward(chain, j):
        block = around(4 * j)
        g_copy(chain, x_buf.at[chain, block], block, t, 0).wait_recv()
        for i, off in enumerate(targets):
            g_copy(chain, x_buf.at[chain, block], block, around(off), 3 * j + i).start()

    def gather_near(chain, j):
        for off in sources:
            block = around(off + 4 * j)
            g_copy(chain, x_buf.at[chain, block], block, t, 0).wait_recv()

    for h in range(HALVES):
        gather_start(h, tokens_ref.at[h])
    for h in range(HALVES):
        x_buf[h, t] = tokens_ref[h]
    own_rows = [tokens_ref[h].astype(F32) for h in range(HALVES)]
    for load in loads:
        load.wait()

    lane8 = iota((8, LANES), 1)
    m8 = (lane8 // HEAD) == (iota((8, LANES), 0) % 2)
    sq = (LANES, LANES)
    same_half = ((iota(sq, 0) // HEAD) == (iota(sq, 1) // HEAD)).astype(F32).astype(BF16)
    spread = ((iota(sq, 0) % 2) == (iota(sq, 1) // HEAD)).astype(F32).astype(BF16)
    collect = ((iota(sq, 0) // HEAD) == (iota(sq, 1) % 2)).astype(F32).astype(BF16)
    tall = (HEAD, LANES)
    row_of = iota(tall, 0)
    lane_of = iota(tall, 1)
    entry = (((lane_of // HEAD) == (row_of % 2)) & (((lane_of % HEAD) // 2) == (row_of // 2))).astype(F32)
    entry = entry.reshape(1, 8, 8, LANES)
    tok_row = iota((rows, LANES), 0)
    live_rows = []
    for h in range(HALVES):
        length_rows = jnp.zeros((rows, LANES), jnp.int32)
        for q in range(seqs):
            length_rows = jnp.where((tok_row // NEW) == q, lengths_ref[h * seqs + q], length_rows)
        live_rows.append((tok_row % NEW) < length_rows)
    groups = rows // 8
    span = LANES // groups

    odd = (t + c) % 2
    even = 1 - odd
    mine = (-odd, odd - even * skip)
    theirs = (-even, even - odd * skip)

    def wave(layer, h, j):
        chain = HALVES * layer + h
        blocks = [around(off + 4 * j) for off in theirs + mine]
        wide = jnp.concatenate([x_buf[chain, block] for block in blocks], 0).astype(F32)
        total = jnp.sum(wide * wide, axis=-1, keepdims=True)
        total = jnp.broadcast_to(total, (4 * rows, LANES)).reshape(4, groups, 8, LANES)
        packed = total[:, 0]
        for g in range(1, groups):
            packed = jnp.where(lane8 // span == g, total[:, g], packed)
        scaled = (wide * gain_ref[pl.ds(layer, 1), :]).astype(BF16)
        for p in range(3):
            out = dot(scaled, w_v[layer, :, 2 * width * p : 2 * width * (p + 1)])
            for k in range(2):
                i = 2 * p + k
                piece = out[:, k * width : (k + 1) * width].reshape(4, rows, width)
                for q in range(2):
                    pair_out[chain, blocks[q] // 2, i * rows : (i + 1) * rows] = piece[q].astype(BF16)
                    own_part[h, blocks[2 + q] // 2, i * rows : (i + 1) * rows] = piece[2 + q]
        for q in range(2):
            pair_out[chain, blocks[q] // 2, 6 * rows :] = pair_rows(packed[q]).astype(BF16)
            own_part[h, blocks[2 + q] // 2, 6 * rows : 6 * rows + 8] = packed[2 + q]
        for q in range(2):
            pair_copy(chain, blocks[q] // 2).start()

    def both(chain, h, place):
        arrived = pair_in[chain, place].astype(F32)
        main = own_part[h, place, : 6 * rows] + arrived[: 6 * rows]
        squares = own_part[h, place, 6 * rows : 6 * rows + 8] + (
            arrived[6 * rows : 6 * rows + 8] + arrived[6 * rows + 8 :]
        )
        return main, squares

    def finish(layer, h, j):
        chain = HALVES * layer + h
        for off in mine:
            place = around(off + 4 * j) // 2
            pair_copy(chain, place).wait_recv()
            main, squares = both(chain, h, place)

            @pl.when(place != x)
            def _():
                rs_out[chain, place, : 6 * rows] = main.astype(BF16)
                rs_out[chain, place, 6 * rows :] = pair_rows(squares).astype(BF16)
                rs_copy(chain, place, x).start()

            @pl.when(place == x)
            def _():
                own_part[h, x, : 6 * rows] = main
                own_part[h, x, 6 * rows : 6 * rows + 8] = squares

    def sum_and_advance(layer, h):
        chain = HALVES * layer + h

        def add_sums(off):
            src = lax.rem(x + off, n_x)
            rs_copy(chain, x, src).wait_recv()
            arrived = rs_in[chain, src].astype(F32)
            own_part[h, x, : 6 * rows] += arrived[: 6 * rows]
            own_part[h, x, 6 * rows : 6 * rows + 8] += arrived[6 * rows : 6 * rows + 8] + arrived[6 * rows + 8 :]

        by_distance(n_x, add_sums)

        squares = own_part[h, x, 6 * rows : 6 * rows + 8]
        inv = lax.rsqrt(squares / model + norm_epsilon)
        inv_rows = jnp.concatenate(
            [jnp.broadcast_to(inv[:, span * g : span * g + 1], (8, LANES)) for g in range(groups)], 0
        )
        recept, keys, values, decay_pre, rate_pre, gate_pre = [
            (inv_rows * own_part[h, x, i * rows : (i + 1) * rows]).astype(BF16).astype(F32) for i in range(6)
        ]
        raw = base_ref[pl.ds(layer, 1), :] + decay_pre
        decays = jnp.exp(-jnp.exp(jnp.float32(-0.5)) / (1.0 + jnp.exp(-raw)))
        rates = 1.0 / (1.0 + jnp.exp(-rate_pre))
        unit = keys * lax.rsqrt(dot_split(keys * keys, same_half) + unit_epsilon)
        zero = jnp.zeros_like(keys)
        decays = jnp.where(live_rows[h], decays, 1.0)
        drop = jnp.where(live_rows[h], unit * rates, zero)
        put = jnp.where(live_rows[h], keys, zero)

        def tile_maker(q):
            turned = pltpu.roll(q, HEAD, 1)

            def tiles(n):
                made = []
                for s in range(seqs):
                    at = NEW * s + n
                    made.append(
                        jnp.where(
                            m8,
                            jnp.broadcast_to(q[at : at + 1], (8, LANES)),
                            jnp.broadcast_to(turned[at : at + 1], (8, LANES)),
                        )
                    )
                return jnp.stack(made)[:, None]

            return tiles

        decay_tiles, unit_tiles, drop_tiles, put_tiles, recept_tiles = [
            tile_maker(q) for q in (decays, unit, drop, put, recept)
        ]
        full = (seqs, 8, 8, LANES)
        flat = (seqs * HEAD, LANES)
        memory = st_v[layer, pl.ds(h * seqs * HEAD, seqs * HEAD)].reshape(full)
        reads = jnp.zeros((rows, LANES), F32)
        for n in range(NEW):
            value_rows = jnp.stack(
                [jnp.broadcast_to(values[NEW * s + n : NEW * s + n + 1], (8, LANES)) for s in range(seqs)]
            )[:, None]
            value_full = dot((value_rows * entry).reshape(flat).astype(BF16), spread).reshape(full)
            removed = dot_split((memory * unit_tiles(n)).reshape(flat), same_half).reshape(full)
            memory = memory * decay_tiles(n) - removed * drop_tiles(n) + value_full * put_tiles(n)
            seen = dot_split((memory * recept_tiles(n)).reshape(flat), collect).reshape(full)
            seen = jnp.sum(seen * entry, axis=1).reshape(seqs * 8, LANES)
            pick_shape = (rows, seqs * 8)
            pick = (iota(pick_shape, 0) == (iota(pick_shape, 1) // 8) * NEW + n).astype(F32).astype(BF16)
            seen_high = seen.astype(BF16)
            seen_low = (seen - seen_high.astype(F32)).astype(BF16)
            reads = reads + dot(pick, seen_high) + dot(pick, seen_low)
        states_out[layer, pl.ds(h * seqs * HEAD, seqs * HEAD)] = memory.reshape(flat)

        mean = dot_split(reads, same_half) / HEAD
        dev = reads - mean
        var = dot_split(dev * dev, same_half) / HEAD
        normed = dev * lax.rsqrt(var + group_epsilon) * group_ref[pl.ds(layer, 1), :]
        mixed = jnp.where(live_rows[h], normed / (1.0 + jnp.exp(-gate_pre)), zero)
        mix_buf[chain, d] = mixed.astype(BF16)

        def send_mixed(off):
            d_copy(chain, lax.rem(d + off, n_dp), d).start()

        by_distance(n_dp, send_mixed)

    def project_out(layer, h):
        chain = HALVES * layer + h
        for j in far_first:
            blocks = [around(off + 4 * j) for off in targets + (0,)]
            for block in blocks:
                @pl.when(block != d)
                def _():
                    d_copy(chain, d, block).wait_recv()

            partial = dot(jnp.concatenate([mix_buf[chain, block] for block in blocks], 0), wo_v[layer])
            partial = partial.reshape(4, rows, feats)
            for i, off in enumerate(targets):
                part_out[chain, blocks[i]] = partial[i].astype(BF16)
                near_copy(chain, j, i, blocks[i], around(off)).start()
            class_sum[h, j] = partial[3]

    def sum_classes(layer, h):
        chain = HALVES * layer + h
        for j in far_first:
            total = class_sum[h, j]
            for i in range(3):
                near_copy(chain, j, i, t, t).wait_recv()
                total = total + part_in[chain, 3 * j + i].astype(F32)
            if j:
                far_out[chain, j] = total.astype(BF16)
                far_copy(chain, j, around(4 * j)).start()
            else:
                own_rows[h] = own_rows[h] + total

    def end_block(layer, h):
        chain = HALVES * layer + h
        for j in near_first[1:]:
            far_copy(chain, j, t).wait_recv()
            own_rows[h] = own_rows[h] + far_in[chain, j].astype(F32)
        done = own_rows[h].astype(BF16)
        if layer == 0:
            x_buf[HALVES + h, t] = done
            gather_start(HALVES + h, x_buf.at[HALVES + h, t])
            own_rows[h] = done.astype(F32)
        else:
            tokens_out[pl.ds(h * rows, rows)] = done

    middle, last = near_first[1:-1], near_first[1:][-1:]
    halves = range(HALVES)
    for layer in range(2):
        chains = [HALVES * layer + h for h in halves]
        for h in halves:
            gather_near(chains[h], 0)
            wave(layer, h, 0)
            for j in middle:
                gather_forward(chains[h], j)
        for h in halves:
            finish(layer, h, 0)
        for j in last:
            for h in halves:
                gather_forward(chains[h], j)
        for h in halves:
            for j in middle:
                gather_near(chains[h], j)
                wave(layer, h, j)
        for h in halves:
            for j in middle:
                finish(layer, h, j)
        for j in last:
            for h in halves:
                gather_near(chains[h], j)
                wave(layer, h, j)
            for h in halves:
                finish(layer, h, j)
        for stage in (sum_and_advance, project_out, sum_classes, end_block):
            for h in halves:
                stage(layer, h)

    for chain in range(2 * HALVES):
        for k in range(n_tp - 1):
            g_copy(chain, tokens_ref.at[0], t, t, k).wait_send()
        for j in range(hops):
            for i in range(3):
                near_copy(chain, j, i, t, t).wait_send()
            if j:
                far_copy(chain, j, t).wait_send()

        def drain_d(off):
            d_copy(chain, lax.rem(d + off, n_dp), d).wait_send()

        def drain_rs(off):
            place = lax.rem(x + off, n_x)
            rs_copy(chain, place, x).wait_send()
            pair_copy(chain, place).wait_send()

        by_distance(n_dp, drain_d)
        by_distance(n_x, drain_rs)
        pair_copy(chain, x).wait_send()


def per_device(n_tp, n_dp, tokens, lengths, norm_gain, w_recept, w_keys, w_values, w_decay, w_rate, w_gate,
               decay_base, group_gain, w_out, states):
    rows, feats = tokens.shape
    layers, seqs, heads, flat = states.shape
    folded = flat // LANES
    width = w_recept.shape[2]
    n_x = n_dp // 2
    state_rows = seqs * folded * heads
    packed = states.reshape(layers, seqs, heads, folded, LANES).transpose(0, 1, 3, 2, 4)
    packed = packed.reshape(layers, state_rows, LANES)
    vmem = pl.BlockSpec(memory_space=pltpu.VMEM)
    hbm = pl.BlockSpec(memory_space=pltpu.HBM)
    part = rows // HALVES
    chains = layers * HALVES
    msg = 6 * part + 16
    out, new_states = pl.pallas_call(
        functools.partial(kernel, n_tp, n_dp),
        out_shape=(
            jax.ShapeDtypeStruct((rows, feats), BF16),
            jax.ShapeDtypeStruct((layers, state_rows, LANES), F32),
        ),
        in_specs=[hbm] * 13,
        out_specs=(vmem, vmem),
        scratch_shapes=[
            pltpu.VMEM((HALVES, part, feats), BF16),
            pltpu.SMEM((seqs,), jnp.int32),
            pltpu.VMEM((layers, feats), F32),
            pltpu.VMEM((layers, width), F32),
            pltpu.VMEM((layers, width), F32),
            pltpu.VMEM((layers, feats, 6 * width), BF16),
            pltpu.VMEM((layers, width, feats), BF16),
            pltpu.VMEM((layers, state_rows, LANES), F32),
            pltpu.VMEM((chains, n_tp, part, feats), BF16),
            pltpu.VMEM((chains, n_x, msg, width), BF16),
            pltpu.VMEM((chains, n_x, msg, width), BF16),
            pltpu.VMEM((HALVES, n_x, msg, width), F32),
            pltpu.VMEM((chains, n_x, msg, width), BF16),
            pltpu.VMEM((chains, n_x, msg, width), BF16),
            pltpu.VMEM((chains, n_dp, part, width), BF16),
            pltpu.VMEM((chains, n_tp, part, feats), BF16),
            pltpu.VMEM((chains, 3 * n_tp // 4, part, feats), BF16),
            pltpu.VMEM((HALVES, n_tp // 4, part, feats), F32),
            pltpu.VMEM((chains, n_tp // 4, part, feats), BF16),
            pltpu.VMEM((chains, n_tp // 4, part, feats), BF16),
            pltpu.SemaphoreType.DMA((14,)),
        ] + [pltpu.SemaphoreType.DMA((chains, n_tp))] * 4
        + [pltpu.SemaphoreType.DMA((chains, n_dp))] * 2
        + [pltpu.SemaphoreType.DMA((chains, n_x))] * 4,
        compiler_params=pltpu.CompilerParams(
            collective_id=0, has_side_effects=True, vmem_limit_bytes=48 * 1024 * 1024
        ),
    )(*[
        pltpu.with_memory_space_constraint(operand, pltpu.HBM)
        for operand in (tokens, lengths, norm_gain, decay_base, group_gain,
                        w_recept, w_keys, w_values, w_decay, w_rate, w_gate, w_out, packed)
    ])
    new_states = new_states.reshape(layers, seqs, folded, heads, LANES).transpose(0, 1, 3, 2, 4)
    return out, new_states.reshape(layers, seqs, heads, flat)


def solution(mesh):
    placed = (
        P(("grp", "tp"), "dp"),
        P(("grp", "dp")),
        P(None, "dp"),
        P(None, "dp", "tp"),
        P(None, "dp", "tp"),
        P(None, "dp", "tp"),
        P(None, "dp", "tp"),
        P(None, "dp", "tp"),
        P(None, "dp", "tp"),
        P(None, "tp"),
        P(None, "tp"),
        P(None, "tp", "dp"),
        P(None, ("grp", "dp"), "tp", None),
    )
    return jax.shard_map(
        functools.partial(per_device, mesh.shape["tp"], mesh.shape["dp"]),
        mesh=mesh,
        in_specs=placed,
        out_specs=(P(("grp", "tp"), "dp"), P(None, ("grp", "dp"), "tp", None)),
        check_vma=False,
    )
```
